128 devices in a mesh: fs: 16 (over z, x), tp: 8 (over y, core).
Axes of the slice: x: 4, y: 4, z: 4, core: 2. Of those that a mesh axis runs over, the one named last changes fastest.
Arguments:
- tokens: bfloat16 [16384, 2048], P(('fs', 'tp')), may hold values from -6 to 6
- gate_weight: bfloat16 [5632, 2048], P('tp', 'fs'), may hold values from -0.125 to 0.125
- up_weight: bfloat16 [5632, 2048], P('tp', 'fs'), may hold values from -0.125 to 0.125
- down_weight: bfloat16 [5632, 2048], P('tp', 'fs'), may hold values from -0.078125 to 0.078125
- out_grad: bfloat16 [16384, 2048], P(('fs', 'tp')), may hold values from -24 to 24
Outputs:
- grad_tokens: bfloat16 [16384, 2048], P(('fs', 'tp'))
- grad_gate: float32 [5632, 2048], P('tp', 'fs')
- grad_up: float32 [5632, 2048], P('tp', 'fs')
- grad_down: float32 [5632, 2048], P('tp', 'fs')
- gate_rows: float32 [5632], P('tp')
- up_rows: float32 [5632], P('tp')
- down_rows: float32 [5632], P('tp')
The draws below stay inside these ranges and needn't reach their ends.
All inputs are finite; a program needn't handle non-finite values.
Results may differ from the reference program's by a relative error of at most 0.014.
Values may be sent and summed in bfloat16 or wider, within the bound.
No kernel may reach another device: no remote copies, remote signals or barrier semaphores. Data moves between devices by JAX's collectives and lax.ppermute only.
A program may use at most 128 MiB of HBM per device.

```python
import math
import jax
import jax.numpy as jnp
from jax import lax

D = 2048
FF = 5632
TOKENS = 16384
N_TP = 8


def with_spikes(values, rng, source, target, blocks, factor):
    def block_of(axis_at):
        return (jnp.arange(values.shape[axis_at]) // (values.shape[axis_at] // blocks)).reshape((-1,) + (1,) * (values.ndim - 1 - axis_at))

    near = jax.random.permutation(rng, blocks)[block_of(target)]
    other_side = (block_of(target) + blocks // 2) % blocks
    return jnp.where((block_of(source) == near) | (block_of(source) == other_side), factor * values, values)


def block_levels(own_key, shape, split, low, high):
    factor_of = 1.0
    for position, parts in split:
        steps = jax.random.uniform(jax.random.fold_in(jax.random.fold_in(own_key, 6), position), (parts,), jnp.float32, low / len(split), high / len(split))
        factor_of = factor_of * jnp.repeat(jnp.exp(steps), shape[position] // parts).reshape((-1,) + (1,) * (len(shape) - 1 - position))
    return factor_of


def noise(key, dims, scale, most, shards=(), dtype=jnp.bfloat16):
    values = scale * jax.random.normal(key, dims, jnp.float32)
    if shards:
        values = values * block_levels(key, dims, shards, -0.22, 0.18)
    return jnp.clip(values, -most, most).astype(dtype)


def bell_draw_with(stream_key, shape, scale, limit, pieces, heavy, held_as=jnp.bfloat16):
    values = scale * jax.random.normal(stream_key, shape, jnp.float32)
    if pieces:
        values = values * block_levels(stream_key, shape, pieces, -0.22, 0.18)
    return jnp.clip(with_spikes(values, jax.random.fold_in(stream_key, 3), *heavy), -limit, limit).astype(held_as)


def setup_inputs(seed: int = 0) -> dict:
    keys = jax.random.split(jax.random.key(seed), 6)
    tokens = noise(keys[0], (TOKENS, D), 1.0, 6.0, ((0, 128),))
    gate_weight = noise(keys[1], (FF, D), D ** -0.5, 0.125, ((0, 8), (1, 16)))
    up_weight = noise(keys[2], (FF, D), D ** -0.5, 0.125, ((0, 8), (1, 16)))
    down_weight = noise(keys[3], (FF, D), FF ** -0.5, 0.078125, ((0, 8), (1, 16)))
    out_grad = bell_draw_with(keys[4], (TOKENS, D), 1.0, 24.0, ((0, 128),), (0, 1, 128, 5.5))
    return {"tokens": tokens, "gate_weight": gate_weight, "up_weight": up_weight, "down_weight": down_weight, "out_grad": out_grad}


def reference(tokens, gate_weight, up_weight, down_weight, out_grad):
    gate = jnp.dot(tokens, gate_weight.T, preferred_element_type=jnp.float32)
    up = jnp.dot(tokens, up_weight.T, preferred_element_type=jnp.float32)
    sig = jax.nn.sigmoid(gate)
    silu = gate * sig
    act = (silu * up).astype(jnp.bfloat16)
    dhidden = jnp.dot(out_grad, down_weight.T, preferred_element_type=jnp.float32)
    dgate = (dhidden * up * sig * (1.0 + gate * (1.0 - sig))).astype(jnp.bfloat16)
    dup = (dhidden * silu).astype(jnp.bfloat16)
    width = FF // N_TP
    total = jnp.zeros((TOKENS, D), jnp.float32)
    for block in range(N_TP):
        lo = block * width
        part = jnp.dot(dgate[:, lo:lo + width], gate_weight[lo:lo + width], preferred_element_type=jnp.float32)
        part = part + jnp.dot(dup[:, lo:lo + width], up_weight[lo:lo + width], preferred_element_type=jnp.float32)
        total = total + lax.optimization_barrier(part.astype(jnp.bfloat16)).astype(jnp.float32)
    grad_tokens = total.astype(jnp.bfloat16)
    factor = 1.0 / math.sqrt(TOKENS)
    grad_gate = jnp.dot(dgate.T, tokens, preferred_element_type=jnp.float32) * factor
    grad_up = jnp.dot(dup.T, tokens, preferred_element_type=jnp.float32) * factor
    grad_down = jnp.dot(act.T, out_grad, preferred_element_type=jnp.float32) * factor
    gate_rows = lax.optimization_barrier(jnp.mean(grad_gate * grad_gate, axis=1))
    up_rows = lax.optimization_barrier(jnp.mean(grad_up * grad_up, axis=1))
    down_rows = lax.optimization_barrier(jnp.mean(grad_down * grad_down, axis=1))
    return (grad_tokens, grad_gate, grad_up, grad_down, gate_rows, up_rows, down_rows)
```

```python
import math

import jax
import jax.numpy as jnp
from jax import lax
from jax.sharding import Mesh, PartitionSpec as P


BF = jnp.bfloat16
F32 = jnp.float32
CUT = 384
FS = ("z", "x")


def hop(x, axis, k):
    return lax.ppermute(x, axis, [(i, (i - k) % 4) for i in range(4)])


def swap(x):
    return lax.ppermute(x, "core", [(0, 1), (1, 0)])


def ring_gather(x, axis, way):
    nxt = hop(x, axis, 1)
    prv = hop(x, axis, -1)
    far = hop(nxt if way > 0 else prv, axis, way)
    return [x, nxt, far, prv]


def ring_scatter(parts, axis, way):
    near, other = (parts[1], parts[3]) if way > 0 else (parts[3], parts[1])
    one = hop(other, axis, way)
    far = hop(parts[2], axis, -way)
    two = hop((near.astype(F32) + far.astype(F32)).astype(BF), axis, -way)
    return parts[0].astype(F32) + one.astype(F32) + two.astype(F32)


def roll_cols(t, z, x):
    n = t.shape[0]
    t = t.reshape(n, 4, 512)
    t = lax.dynamic_slice_in_dim(jnp.concatenate([t, t], axis=1), z, 4, axis=1)
    t = t.reshape(n, 4, 4, 128)
    t = lax.dynamic_slice_in_dim(jnp.concatenate([t, t], axis=2), x, 4, axis=2)
    return t.reshape(n, 2048)


def gather_rows(t, way):
    mine = jnp.concatenate(ring_gather(t, "y", way), axis=0)
    return jnp.concatenate([mine, swap(mine)], axis=0)


def dot(a, b, ca, cb):
    return lax.dot_general(a, b, (((ca,), (cb,)), ((), ())), preferred_element_type=F32)


def mean_rows(s):
    v = jnp.sum(s * s, axis=0)
    v = lax.all_to_all(jnp.broadcast_to(v[None], (16, v.size)), FS, 0, 0, tiled=True)
    return jnp.sum(v, axis=0) / 2048.0


def body(tokens, gate_weight, up_weight, down_weight, out_grad):
    tok = gather_rows(tokens, 1)
    og = gather_rows(out_grad, -1)
    w = jnp.concatenate([gate_weight, up_weight, down_weight], axis=0)
    w = lax.all_gather(w, FS, axis=1, tiled=True)
    n = 704
    gate, up = dot(w[:n], tok, 1, 1), dot(w[n : 2 * n], tok, 1, 1)
    sig = jax.nn.sigmoid(gate)
    silu = gate * sig
    act = (silu * up).astype(BF)
    dhidden = dot(w[2 * n :], og, 1, 1)
    dgate = (dhidden * up * sig * (1.0 + gate * (1.0 - sig))).astype(BF)
    dup = (dhidden * silu).astype(BF)
    factor = 1.0 / math.sqrt(16384.0)
    d = jnp.concatenate([dgate, dup], axis=0)
    part = jnp.concatenate(
        [(dot(tok, d, 0, 1) * factor).astype(BF), (dot(og, act, 0, 1) * factor).astype(BF)], axis=1
    )
    s = lax.psum_scatter(part, FS, scatter_dimension=0, tiled=True).astype(F32)
    gt = dot(d, w[: 2 * n], 0, 0).astype(BF).reshape(2, 4, 128, 2048)
    gt = (gt[0].astype(F32) + swap(gt[1]).astype(F32)).astype(BF)
    gt = ring_scatter([gt[k] for k in range(4)], "y", 1).astype(BF)
    r = mean_rows(s)
    t = s.T
    return (gt, t[:n], t[n : 2 * n], t[2 * n :], r[:n], r[n : 2 * n], r[2 * n :])


def solution(mesh):
    fine = Mesh(mesh.devices.reshape(4, 4, 4, 2), ("z", "x", "y", "core"))
    tp = ("y", "core")
    return jax.shard_map(
        body,
        mesh=fine,
        in_specs=(P(FS + tp, None), P(tp, FS), P(tp, FS), P(tp, FS), P(FS + tp, None)),
        out_specs=(P(FS + tp, None), P(tp, FS), P(tp, FS), P(tp, FS), P(tp), P(tp), P(tp)),
        check_vma=False,
    )
```
